32 devices in a mesh: ep: 8 (over z, x), tp: 4 (over y, core).
Axes of the slice: x: 2, y: 2, z: 4, core: 2. Of those that a mesh axis runs over, the one named last changes fastest.
Arguments:
- query_rows: bfloat16 [2048, 1024], P('ep', 'tp'), may hold values from -8 to 8
- key_rows: bfloat16 [2048, 256], P('ep', 'tp'), may hold values from -8 to 8
- value_rows: bfloat16 [2048, 256], P('ep', 'tp'), may hold values from -16 to 16
- query_gain: float32 [64], replicated, may hold values from 0.5 to 7.5
- key_gain: float32 [64], replicated, may hold values from 0.5 to 7.5
- moe_tokens: bfloat16 [4096, 2048], P(('ep', 'tp')), may hold values from -6 to 6
- norm_gain: float32 [2048], replicated, may hold values from 0.1 to 1.9
- routes: int32 [4096, 2], P('ep'), may hold values from 0 to 7, all different within a row; in each aligned block of 128 rows (0 to 127, 128 to 255, ...) at most 64 rows name the same one
- route_weights: float32 [4096, 2], P('ep'), may hold values from 0.1 to 1
- expert_gate: bfloat16 [8, 2048, 1024], P('ep', None, 'tp'), may hold values from -0.125 to 0.125
- expert_up: bfloat16 [8, 2048, 1024], P('ep', None, 'tp'), may hold values from -0.125 to 0.125
- expert_down: bfloat16 [8, 1024, 2048], P('ep', 'tp'), may hold values from -0.1875 to 0.1875
- shared_gate: bfloat16 [2048, 1024], P(None, 'tp'), may hold values from -0.125 to 0.125
- shared_up: bfloat16 [2048, 1024], P(None, 'tp'), may hold values from -0.125 to 0.125
- shared_down: bfloat16 [1024, 2048], P('tp'), may hold values from -0.1875 to 0.1875
Outputs:
- attn_out: bfloat16 [2048, 1024], P('ep', 'tp')
- moe_out: bfloat16 [4096, 2048], P(('ep', 'tp'))
The draws below stay inside these ranges and needn't reach their ends.
Inputs may be any that keep to these rules, and one draw needn't show every extreme that they name: `routes`: each row names 2 different experts. Within each aligned block of 128 rows no expert is named more than 64 times, and in every draw some expert is named exactly 64 times in some block.
All inputs are finite; a program needn't handle non-finite values.
Results may differ from the reference program's by a relative error of at most 0.012.
The reference program's roundings to bfloat16 on the way count: a program that leaves them out, or rounds other values in their place, can miss the bound.
Values may be sent and summed in bfloat16 or wider, within the bound.
A program may use at most 192 MiB of HBM per device.

```python
import math
import jax
import jax.numpy as jnp
import numpy as np
from jax import lax

D = 2048
HEADS = 16
KV_HEADS = 4
HD = 64
F = 1024
TOP = 2
GRID_W = 64
TOK_B = 128
TOKENS_A = 2048
TOKENS_B = 4096
EXPERTS = 8
CAP = 64
N_TP = 4


def draw_key_rows(key, part):
    result = jnp.clip(jax.random.normal(jax.random.fold_in(key, 72), (TOKENS_A, KV_HEADS * HD), jnp.float32), -6.0, 6.0)
    return result.astype(jnp.bfloat16)


def draw_query_rows(key, part):
    result = jnp.clip(jax.random.normal(jax.random.fold_in(key, 73), (TOKENS_A, HEADS * HD), jnp.float32), -6.0, 6.0)
    return result.astype(jnp.bfloat16)


def gain_draw(key, salt):
    result = jax.random.uniform(jax.random.fold_in(key, salt + 3), (HD,), jnp.float32, 1.2, 1.8)
    return result


def draw_query_gain(key, part):
    return gain_draw(key, 80)


def draw_key_gain(key, part):
    return gain_draw(key, 90)


def level_of(key, dims, pieces, low, top_value):
    factor_of, own = 1.0, jax.random.fold_in(key, 6)
    for axis_at, blocks in pieces:
        heights = jnp.exp(jax.random.uniform(jax.random.fold_in(own, axis_at), (blocks,), jnp.float32, low / len(pieces), top_value / len(pieces)))
        factor_of = factor_of * jnp.repeat(heights, dims[axis_at] // blocks).reshape([-1 if axis == axis_at else 1 for axis in range(len(dims))])
    return factor_of


def assign_block(stream_key, own, number, rows, amount, top, bound, slope):
    ranking = jax.random.permutation(stream_key, amount)
    crowded, common = portions_of(amount, rows * top, bound, slope, True), portions_of(amount, rows * top, bound, slope, False)
    places = jnp.arange(amount)

    def named(sizes, rotation):
        used = int((sizes > 0).sum())
        fixed = max(1, used // 4)
        passed = fixed + (places - fixed + rotation * (used - fixed)) % max(1, amount - fixed)
        return jnp.zeros((amount,), jnp.int32).at[ranking[jnp.where(places < fixed, places, passed)]].set(jnp.asarray(sizes, jnp.int32))

    sizes = jnp.where(number % 4 == 0, named(crowded, number // 4), named(common, number - number // 4 - 1))
    mixed = jax.random.permutation(jax.random.fold_in(own, 3), amount)
    source_of, receiver = mixed[0:amount // 2 * 2:2], mixed[1:amount // 2 * 2:2]
    room = jnp.minimum(sizes[source_of] - 1, bound - sizes[receiver]) // 2
    room = jnp.where((source_of == ranking[0]) | (receiver == ranking[0]) | (sizes[receiver] == 0), 0, jnp.maximum(room, 0))
    passed = jax.random.randint(jax.random.fold_in(own, 4), (amount // 2,), 0, 1 << 20) % (room + 1)
    sizes = sizes.at[source_of].add(-passed).at[receiver].add(passed)
    items = jnp.searchsorted(jnp.cumsum(sizes), jnp.arange(rows * top), side="right").astype(jnp.int32)
    table = items.reshape(top, rows).T
    table = table[jax.random.permutation(jax.random.fold_in(own, 1), rows)]
    rotation = jax.random.randint(jax.random.fold_in(own, 2), (rows, 1), 0, top)
    return jnp.take_along_axis(table, (jnp.arange(top)[None, :] + rotation) % top, axis=1)


def portions_of(number_of, total, limit, skew, full):
    weights = [(1 << 20) // math.isqrt(standing ** skew) + 1 for standing in range(1, number_of + 1)]
    largest = limit if full else min(limit, max(-(-total // number_of), total * weights[0] // sum(weights)))
    least = 1 if total - largest >= number_of - 1 else 0
    holding, surplus = [largest] + [least] * (number_of - 1), total - largest - least * (number_of - 1)
    while surplus > 0:
        movable = [i for i in range(1, number_of) if holding[i] < largest] or [i for i in range(1, number_of) if holding[i] < limit]
        pool, remaining = sum([weights[i] for i in movable]), surplus
        for i in movable:
            more = min(limit - holding[i], max(1, remaining * weights[i] // pool), surplus)
            holding[i] = holding[i] + more
            surplus = surplus - more
    return np.array(holding)


def gaussian(key, extent, width, reach, pieces=(), kind=jnp.bfloat16):
    entries = width * jax.random.normal(key, extent, jnp.float32)
    if pieces:
        entries = entries * level_of(key, extent, pieces, -0.22, 0.18)
    return jnp.clip(entries, -reach, reach).astype(kind)


def setup_inputs(seed: int = 0) -> dict:
    key_list = jax.random.split(jax.random.key(seed), 16)
    query_rows = draw_query_rows(jax.random.fold_in(key_list[15], 71), 0)
    key_rows = draw_key_rows(jax.random.fold_in(key_list[15], 71), 0)
    value_rows = gaussian(key_list[2], (TOKENS_A, KV_HEADS * HD), 3.0, 16.0, ((0, 8), (1, 4)))
    query_gain = draw_query_gain(jax.random.fold_in(key_list[15], 71), 0)
    key_gain = draw_key_gain(jax.random.fold_in(key_list[15], 71), 0)
    moe_tokens = gaussian(key_list[5], (TOKENS_B, D), 1.0, 6.0, ((0, 32),))
    norm_gain = jnp.clip(1.0 + 0.18 * jax.random.normal(key_list[6], (D,), jnp.float32), 0.1, 1.9)
    routes_keys = jax.random.split(jax.random.fold_in(key_list[7], 1), TOKENS_B // TOK_B)
    routes_turns = jax.random.permutation(jax.random.fold_in(key_list[7], 3), TOKENS_B // TOK_B)
    routes = jax.vmap(lambda own, number: assign_block(jax.random.fold_in(key_list[7], 2), own, number, TOK_B, EXPERTS, TOP, CAP, 1))(routes_keys, routes_turns).reshape((TOKENS_B, TOP))
    route_weights = jnp.clip(0.1 + 0.9 * jax.random.uniform(key_list[8], (TOKENS_B, TOP), jnp.float32) ** level_of(key_list[8], (TOKENS_B, TOP), ((0, 8),), -0.2, 0.2), 0.1, 1.0)
    expert_gate = gaussian(key_list[9], (EXPERTS, D, F), D ** -0.5, 0.125, ((0, 8), (2, 4)))
    expert_up = gaussian(key_list[10], (EXPERTS, D, F), D ** -0.5, 0.125, ((0, 8), (2, 4)))
    expert_down = gaussian(key_list[11], (EXPERTS, F, D), F ** -0.5, 0.1875, ((0, 8), (1, 4)))
    shared_gate = gaussian(key_list[12], (D, F), D ** -0.5, 0.125, ((1, 4),))
    shared_up = gaussian(key_list[13], (D, F), D ** -0.5, 0.125, ((1, 4),))
    shared_down = gaussian(key_list[14], (F, D), F ** -0.5, 0.1875, ((0, 4),))
    return {"query_rows": query_rows, "key_rows": key_rows, "value_rows": value_rows, "query_gain": query_gain, "key_gain": key_gain, "moe_tokens": moe_tokens, "norm_gain": norm_gain, "routes": routes, "route_weights": route_weights, "expert_gate": expert_gate, "expert_up": expert_up, "expert_down": expert_down, "shared_gate": shared_gate, "shared_up": shared_up, "shared_down": shared_down}


epsilon = 1e-06
rotary_base = 10000.0
routed_scale = 2.5

def rotate_heads(heads_in, gain_row, positions):
    values32 = heads_in.astype(jnp.float32)
    scaled = values32 * lax.rsqrt(lax.optimization_barrier(jnp.mean(values32 * values32, axis=-1, keepdims=True)) + epsilon) * gain_row
    pair_count = scaled.shape[-1] // 4
    inv_freq = rotary_base ** (-jnp.arange(pair_count, dtype=jnp.float32) / pair_count)
    grid_row = (positions // GRID_W).astype(jnp.float32)
    grid_col = (positions % GRID_W).astype(jnp.float32)
    angles = jnp.concatenate([grid_row[:, None] * inv_freq, grid_col[:, None] * inv_freq], axis=-1)[:, None, :]
    cosine = jnp.cos(angles)
    sine_part = jnp.sin(angles)
    first_half = scaled[..., 0::2]
    second_half = scaled[..., 1::2]
    turned = jnp.stack([first_half * cosine - second_half * sine_part, first_half * sine_part + second_half * cosine], axis=-1)
    return turned.reshape(scaled.shape).astype(jnp.bfloat16)

def attention(query_rows, key_rows, value_rows, query_gain, key_gain):
    token_count = query_rows.shape[0]
    group = HEADS // KV_HEADS
    positions = jnp.arange(token_count, dtype=jnp.int32)
    q_rot = rotate_heads(query_rows.reshape(token_count, HEADS, HD), query_gain, positions)
    k_rot = rotate_heads(key_rows.reshape(token_count, KV_HEADS, HD), key_gain, positions)
    keys32 = lax.optimization_barrier(k_rot).astype(jnp.float32)
    values32 = value_rows.reshape(token_count, KV_HEADS, HD).astype(jnp.float32)
    block_len = math.gcd(token_count, 256)
    q_blocks = lax.optimization_barrier(q_rot).reshape(token_count // block_len, block_len, KV_HEADS, group, HD)

    def one_block(q_block):
        scores = jnp.einsum('qgrd,sgd->qgrs', q_block.astype(jnp.float32), keys32) * HD ** (-0.5)
        row_max = lax.optimization_barrier(jnp.max(scores, axis=-1, keepdims=True))
        weights = jnp.exp(scores - row_max)
        row_sum = lax.optimization_barrier(jnp.sum(weights, axis=-1, keepdims=True))
        rounded = lax.optimization_barrier(weights.astype(jnp.bfloat16)).astype(jnp.float32)
        mixed = jnp.einsum('qgrs,sgd->qgrd', rounded, values32)
        return (mixed / row_sum).astype(jnp.bfloat16)
    result = lax.map(one_block, q_blocks)
    return result.reshape(token_count, HEADS * HD)

def feed_forward(rows_in, w_gate, w_up, w_down):
    gate_proj = jnp.dot(rows_in, w_gate, preferred_element_type=jnp.float32)
    up_proj = jnp.dot(rows_in, w_up, preferred_element_type=jnp.float32)
    hidden = lax.optimization_barrier((jax.nn.silu(gate_proj) * up_proj).astype(jnp.bfloat16))
    block_width = hidden.shape[-1] // N_TP
    summed = jnp.zeros((rows_in.shape[0], w_down.shape[1]), jnp.float32)
    for part_index in range(N_TP):
        lower = part_index * block_width
        partial_sum = jnp.dot(hidden[:, lower:lower + block_width], w_down[lower:lower + block_width], preferred_element_type=jnp.float32).astype(jnp.bfloat16)
        summed = summed + lax.optimization_barrier(partial_sum).astype(jnp.float32)
    return summed

def mixture(moe_tokens, norm_gain, routes, route_weights, expert_gate, expert_up, expert_down, shared_gate, shared_up, shared_down):
    total_rows = moe_tokens.shape[0]
    blocks = total_rows // TOK_B
    values32 = moe_tokens.astype(jnp.float32)
    normed = (values32 * lax.rsqrt(lax.optimization_barrier(jnp.mean(values32 * values32, axis=-1, keepdims=True)) + epsilon) * norm_gain).astype(jnp.bfloat16)
    normed = lax.optimization_barrier(normed)
    gates = route_weights / lax.optimization_barrier(jnp.sum(route_weights, axis=-1, keepdims=True)) * routed_scale
    chosen = routes.reshape(blocks, TOK_B * TOP).astype(jnp.int32)
    one_hot = (chosen[:, :, None] == jnp.arange(EXPERTS, dtype=jnp.int32)[None, None, :]).astype(jnp.int32)
    ranks = lax.optimization_barrier(jnp.sum((jnp.cumsum(one_hot, axis=1) - one_hot) * one_hot, axis=2))
    block_ids = jnp.arange(blocks, dtype=jnp.int32)[:, None]
    dest = (chosen * blocks + block_ids) * CAP + ranks
    rows_from = block_ids * TOK_B + jnp.arange(TOK_B * TOP, dtype=jnp.int32)[None, :] // TOP
    slot_rows = jnp.full((EXPERTS * blocks * CAP,), total_rows, jnp.int32).at[dest.reshape(-1)].set(rows_from.reshape(-1))
    padded = jnp.concatenate([normed, jnp.zeros((1, D), jnp.bfloat16)], axis=0)

    def one_expert(inputs):
        index_rows, w_gate, w_up, w_down = inputs
        return feed_forward(padded[index_rows], w_gate, w_up, w_down).astype(jnp.bfloat16)
    expert_rows = lax.map(one_expert, (slot_rows.reshape(EXPERTS, blocks * CAP), expert_gate, expert_up, expert_down))
    flat_rows = lax.optimization_barrier(expert_rows.reshape(EXPERTS * blocks * CAP, D))
    picked = flat_rows[dest.reshape(-1)].astype(jnp.float32).reshape(total_rows, TOP, D)
    routed = lax.optimization_barrier(jnp.sum(gates[:, :, None] * picked, axis=1))
    shared = feed_forward(normed, shared_gate, shared_up, shared_down)
    return (routed + shared).astype(jnp.bfloat16)

def reference(query_rows, key_rows, value_rows, query_gain, key_gain, moe_tokens, norm_gain, routes, route_weights, expert_gate, expert_up, expert_down, shared_gate, shared_up, shared_down):
    attn_out = attention(query_rows, key_rows, value_rows, query_gain, key_gain)
    moe_out = mixture(moe_tokens, norm_gain, routes, route_weights, expert_gate, expert_up, expert_down, shared_gate, shared_up, shared_down)
    return (attn_out, moe_out)
```

```python
import functools

import jax
import jax.numpy as jnp
from jax import lax
from jax.experimental import pallas as pl
from jax.experimental.pallas import tpu as pltpu
from jax.sharding import PartitionSpec as P

GRID_W = 64
MESH = pl.DeviceIdType.MESH


epsilon = 1e-06
rotary_base = 10000.0
routed_scale = 2.5


def exchange_kernel(plan, sizes, *refs):
    count = len(plan)
    sources, targets = refs[:count], refs[count : 2 * count]
    send_sems = refs[2 * count : 3 * count]
    recv_sems = refs[3 * count : 4 * count]
    own_sems = refs[4 * count]
    axes = []
    for axis, _ in plan:
        if axis not in axes:
            axes.append(axis)
    barrier = pltpu.get_barrier_semaphore()
    for axis in axes:
        me, n = lax.axis_index(axis), sizes[axis]

        def greet(i, c, axis=axis, me=me, n=n):
            pl.semaphore_signal(
                barrier, inc=1, device_id={axis: lax.rem(me + i, n)}, device_id_type=MESH
            )
            return c

        lax.fori_loop(1, n, greet, 0)
    pl.semaphore_wait(barrier, sum(sizes[axis] - 1 for axis in axes))

    def copy_of(k, i):
        axis, scattered = plan[k]
        me, n = lax.axis_index(axis), sizes[axis]
        peer = lax.rem(me + i, n)
        return pltpu.make_async_remote_copy(
            src_ref=sources[k].at[peer] if scattered else sources[k],
            dst_ref=targets[k].at[me],
            send_sem=send_sems[k].at[i],
            recv_sem=recv_sems[k].at[i],
            device_id={axis: peer},
            device_id_type=MESH,
        )

    for k, (axis, scattered) in enumerate(plan):

        def begin(i, c, k=k):
            copy_of(k, i).start()
            return c

        lax.fori_loop(1, sizes[axis], begin, 0)
    local = []
    for k, (axis, scattered) in enumerate(plan):
        me = lax.axis_index(axis)
        copy = pltpu.make_async_copy(
            sources[k].at[me] if scattered else sources[k], targets[k].at[me], own_sems.at[k]
        )
        copy.start()
        local.append(copy)
    for copy in local:
        copy.wait()
    for k, (axis, scattered) in enumerate(plan):

        def finish(i, c, k=k):
            copy_of(k, i).wait()
            return c

        lax.fori_loop(1, sizes[axis], finish, 0)


def exchange(operands, plan, number):
    sizes = {axis: lax.axis_size(axis) for axis, _ in plan}
    shapes = []
    for array, (axis, scattered) in zip(operands, plan):
        shape = array.shape if scattered else (sizes[axis],) + array.shape
        shapes.append(jax.ShapeDtypeStruct(shape, array.dtype))
    sems = [pltpu.SemaphoreType.DMA((sizes[axis],)) for axis, _ in plan]
    traffic = 2 * sum(s.size * s.dtype.itemsize for s in shapes)
    return pl.pallas_call(
        functools.partial(exchange_kernel, plan, sizes),
        out_shape=shapes,
        in_specs=[pl.BlockSpec(memory_space=pl.ANY)] * len(plan),
        out_specs=[pl.BlockSpec(memory_space=pl.ANY)] * len(plan),
        scratch_shapes=sems + sems + [pltpu.SemaphoreType.DMA((len(plan),))],
        compiler_params=pltpu.CompilerParams(collective_id=number, has_side_effects=True),
        cost_estimate=pl.CostEstimate(
            flops=0, bytes_accessed=16 * traffic, transcendentals=0
        ),
    )(*operands)


def rotate_heads(heads_in, gain_row, positions):
    values32 = heads_in.astype(jnp.float32)
    scaled = (
        values32
        * lax.rsqrt(jnp.mean(values32 * values32, axis=-1, keepdims=True) + epsilon)
        * gain_row
    )
    pair_count = scaled.shape[-1] // 4
    inv_freq = rotary_base ** (-jnp.arange(pair_count, dtype=jnp.float32) / pair_count)
    grid_row = (positions // GRID_W).astype(jnp.float32)
    grid_col = (positions % GRID_W).astype(jnp.float32)
    angles = jnp.concatenate([grid_row[:, None] * inv_freq, grid_col[:, None] * inv_freq], axis=-1)[
        :, None, :
    ]
    cosine = jnp.cos(angles)
    sine_part = jnp.sin(angles)
    first_half = scaled[..., 0::2]
    second_half = scaled[..., 1::2]
    turned = jnp.stack(
        [
            first_half * cosine - second_half * sine_part,
            first_half * sine_part + second_half * cosine,
        ],
        axis=-1,
    )
    return turned.reshape(scaled.shape).astype(jnp.bfloat16)


def span_length(row_count):
    length = min(row_count, 2048)
    while row_count % length:
        length -= 1
    return length


def rotated(query_rows, key_rows, value_rows, query_gain, key_gain):
    row_count = query_rows.shape[0]
    head_size = query_gain.shape[0]
    q_heads = query_rows.shape[1] // head_size
    kv_heads = key_rows.shape[1] // head_size
    positions = lax.axis_index("ep") * row_count + jnp.arange(row_count, dtype=jnp.int32)
    q_rot = rotate_heads(query_rows.reshape(row_count, q_heads, head_size), query_gain, positions)
    k_rot = rotate_heads(key_rows.reshape(row_count, kv_heads, head_size), key_gain, positions)
    key_value = jnp.stack([k_rot, value_rows.reshape(row_count, kv_heads, head_size)], axis=2)
    return q_rot, key_value.reshape(row_count, kv_heads * 2 * head_size)


def attend(q_rot, piece_rows):
    row_count, q_heads, head_size = q_rot.shape
    kv_heads = piece_rows.shape[1] // (2 * head_size)
    group = q_heads // kv_heads
    scale = head_size ** (-0.5)
    q_grouped = q_rot.reshape(row_count, kv_heads, group, head_size).transpose(1, 2, 0, 3)
    q_grouped = q_grouped.reshape(kv_heads, group * row_count, head_size)
    query_count = group * row_count
    initial = (
        jnp.full((kv_heads, query_count), -jnp.inf, jnp.float32),
        jnp.zeros((kv_heads, query_count), jnp.float32),
        jnp.zeros((kv_heads, query_count, head_size), jnp.float32),
    )

    def one_span(carried, span_rows):
        run_max, run_sum, mixed = carried
        keys_span = span_rows[:, :, 0, :]
        values_span = span_rows[:, :, 1, :]
        scores = (
            jnp.einsum("hrd,shd->hrs", q_grouped, keys_span, preferred_element_type=jnp.float32)
            * scale
        )
        new_max = jnp.maximum(run_max, jnp.max(scores, axis=-1))
        factor = jnp.exp(run_max - new_max)
        weights = jnp.exp(scores - new_max[..., None])
        run_sum = run_sum * factor + jnp.sum(weights, axis=-1)
        added = jnp.einsum(
            "hrs,shd->hrd",
            weights.astype(jnp.bfloat16),
            values_span,
            preferred_element_type=jnp.float32,
        )
        mixed = mixed * factor[..., None] + added
        return ((new_max, run_sum, mixed), None)

    piece_count = piece_rows.shape[0]
    length = span_length(piece_count)
    spans = piece_rows.reshape(piece_count // length, length, kv_heads, 2, head_size)
    carried, unused = lax.scan(one_span, initial, spans)
    run_max, run_sum, mixed = carried
    result = (mixed / run_sum[..., None]).astype(jnp.bfloat16)
    result = result.reshape(kv_heads, group, row_count, head_size).transpose(2, 0, 1, 3)
    return result.reshape(row_count, q_heads * head_size)


def slot_numbers(own_routes, experts, capacity):
    tok_rows = own_routes.shape[0]
    named = own_routes[:, :, None] == jnp.arange(experts, dtype=jnp.int32)
    counts = jnp.any(named, axis=1).astype(jnp.bfloat16)
    rows = jnp.arange(tok_rows, dtype=jnp.int32)
    before = (rows[:, None] > rows[None, :]).astype(jnp.bfloat16)
    earlier = jnp.dot(before, counts, preferred_element_type=jnp.float32)
    ranks = jnp.sum(jnp.where(named, earlier[:, None, :], 0.0), axis=2).astype(jnp.int32)
    return own_routes * capacity + ranks


def hidden_of(rows_in, w_gate, w_up):
    gate_proj = jnp.einsum("...rd,...df->...rf", rows_in, w_gate, preferred_element_type=jnp.float32)
    up_proj = jnp.einsum("...rd,...df->...rf", rows_in, w_up, preferred_element_type=jnp.float32)
    return (jax.nn.silu(gate_proj) * up_proj).astype(jnp.bfloat16)


def body(
    query_rows,
    key_rows,
    value_rows,
    query_gain,
    key_gain,
    moe_tokens,
    norm_gain,
    routes,
    route_weights,
    expert_gate,
    expert_up,
    expert_down,
    shared_gate,
    shared_up,
    shared_down,
):
    tok_rows, model_width = moe_tokens.shape
    top_count = routes.shape[1]
    tp_size = lax.axis_size("tp")
    ep_size = lax.axis_size("ep")
    local_experts = expert_gate.shape[0]
    experts = local_experts * ep_size
    capacity = 2 * tok_rows * top_count // experts
    lane = lax.axis_index("tp")

    all_gate = lax.all_gather(expert_gate, "tp", axis=0)
    all_up = lax.all_gather(expert_up, "tp", axis=0)
    all_down = lax.all_gather(expert_down, "tp", axis=0)

    values32 = moe_tokens.astype(jnp.float32)
    normed = (
        values32
        * lax.rsqrt(jnp.mean(values32 * values32, axis=-1, keepdims=True) + epsilon)
        * norm_gain
    ).astype(jnp.bfloat16)
    own_routes = lax.dynamic_slice_in_dim(routes, lane * tok_rows, tok_rows, 0)
    own_weights = lax.dynamic_slice_in_dim(route_weights, lane * tok_rows, tok_rows, 0)
    own_gates = own_weights / jnp.sum(own_weights, axis=-1, keepdims=True) * routed_scale
    slots = slot_numbers(own_routes, experts, capacity)
    slot_ids = jnp.arange(experts * capacity, dtype=jnp.int32)
    placing = jnp.any(slot_ids[:, None, None] == slots[None, :, :], axis=2).astype(jnp.bfloat16)
    send = jnp.dot(placing, normed, preferred_element_type=jnp.float32).astype(jnp.bfloat16)
    send = send.reshape(ep_size, local_experts * capacity, model_width)

    q_rot, key_value = rotated(query_rows, key_rows, value_rows, query_gain, key_gain)

    arrived, group_rows, pieces = exchange(
        (send, normed, key_value), (("ep", True), ("tp", False), ("ep", False)), 1
    )
    attn_out = attend(q_rot, pieces.reshape(-1, pieces.shape[-1]))
    shared_hidden = hidden_of(
        group_rows.reshape(tp_size * tok_rows, model_width), shared_gate, shared_up
    )
    shared_part = jnp.dot(shared_hidden, shared_down, preferred_element_type=jnp.float32)
    shared_part = shared_part.astype(jnp.bfloat16).reshape(tp_size, tok_rows, model_width)

    arrived = arrived.reshape(ep_size, local_experts, capacity, model_width).transpose(1, 0, 2, 3)
    arrived = arrived.reshape(local_experts, ep_size * capacity, model_width)
    total = 0.0
    for part in range(tp_size):
        hidden = hidden_of(arrived, all_gate[part], all_up[part])
        partial = jnp.einsum(
            "lrf,lfd->lrd", hidden, all_down[part], preferred_element_type=jnp.float32
        )
        total = total + partial.astype(jnp.bfloat16).astype(jnp.float32)
    outgoing = total.astype(jnp.bfloat16).reshape(local_experts, ep_size, capacity, model_width)
    outgoing = outgoing.transpose(1, 0, 2, 3).reshape(
        ep_size, local_experts * capacity, model_width
    )
    returned, shared_parts = exchange((outgoing, shared_part), (("ep", True), ("tp", True)), 2)

    flat_rows = returned.reshape(experts * capacity, model_width)
    moe_out = jnp.sum(shared_parts.astype(jnp.float32), axis=0)
    for k in range(top_count):
        choosing = (slots[:, k, None] == slot_ids[None, :]).astype(jnp.bfloat16)
        picked = jnp.dot(choosing, flat_rows, preferred_element_type=jnp.float32)
        moe_out = moe_out + own_gates[:, k, None] * picked
    return (attn_out, moe_out.astype(jnp.bfloat16))


def solution(mesh):
    return jax.shard_map(
        body,
        mesh=mesh,
        in_specs=(
            P("ep", "tp"),
            P("ep", "tp"),
            P("ep", "tp"),
            P(),
            P(),
            P(("ep", "tp"), None),
            P(),
            P("ep", None),
            P("ep", None),
            P("ep", None, "tp"),
            P("ep", None, "tp"),
            P("ep", "tp", None),
            P(None, "tp"),
            P(None, "tp"),
            P("tp", None),
        ),
        out_specs=(P("ep", "tp"), P(("ep", "tp"), None)),
        check_vma=False,
    )
```

```python
import functools

import jax
import jax.numpy as jnp
from jax import lax
from jax.experimental import pallas as pl
from jax.experimental.pallas import tpu as pltpu
from jax.sharding import PartitionSpec as P

GRID_W = 64
MESH = pl.DeviceIdType.MESH


epsilon = 1e-06
rotary_base = 10000.0
routed_scale = 2.5


def flip(number, mask):
    result, bit = number, 1
    while bit <= mask:
        if mask & bit:
            result = result + bit - 2 * bit * lax.rem(lax.div(number, bit), 2)
        bit *= 2
    return result


def doubled(blocks, axis):
    n = lax.axis_size(axis)
    masks, step = [0], n // 2
    while step:
        pairs = [(j, j ^ step) for j in range(n)]
        blocks = blocks + [lax.ppermute(block, axis, pairs) for block in blocks]
        masks = masks + [mask ^ step for mask in masks]
        step //= 2
    return blocks, masks


def each_peer(axis, sizes, step):
    if axis == "tp":
        for i in range(1, sizes[axis]):
            step(i, 0)
    else:
        lax.fori_loop(1, sizes[axis], step, 0)


def exchange_kernel(plan, sizes, *refs):
    count = len(plan)
    sources, targets = refs[:count], refs[count : 2 * count]
    send_sems = refs[2 * count : 3 * count]
    recv_sems = refs[3 * count : 4 * count]
    own_sems = refs[4 * count]
    axes = []
    for axis, _ in plan:
        if axis not in axes:
            axes.append(axis)
    barrier = pltpu.get_barrier_semaphore()
    for axis in axes:
        me, n = lax.axis_index(axis), sizes[axis]

        def greet(i, c, axis=axis, me=me, n=n):
            pl.semaphore_signal(
                barrier, inc=1, device_id={axis: lax.rem(me + i, n)}, device_id_type=MESH
            )
            return c

        lax.fori_loop(1, n, greet, 0)
    pl.semaphore_wait(barrier, sum(sizes[axis] - 1 for axis in axes))

    def copy_of(k, i):
        axis, scattered = plan[k]
        me, n = lax.axis_index(axis), sizes[axis]
        if axis == "tp":
            peer, source_at, target_at = flip(me, i), i, i
        else:
            peer = lax.rem(me + i, n)
            source_at, target_at = peer, me
        return pltpu.make_async_remote_copy(
            src_ref=sources[k].at[source_at] if scattered else sources[k],
            dst_ref=targets[k].at[target_at],
            send_sem=send_sems[k].at[i],
            recv_sem=recv_sems[k].at[i],
            device_id={axis: peer},
            device_id_type=MESH,
        )

    for k, (axis, scattered) in enumerate(plan):

        def begin(i, c, k=k):
            copy_of(k, i).start()
            return c

        each_peer(axis, sizes, begin)
    local = []
    for k, (axis, scattered) in enumerate(plan):
        me = 0 if axis == "tp" else lax.axis_index(axis)
        copy = pltpu.make_async_copy(
            sources[k].at[me] if scattered else sources[k], targets[k].at[me], own_sems.at[k]
        )
        copy.start()
        local.append(copy)
    for copy in local:
        copy.wait()
    for k, (axis, scattered) in enumerate(plan):

        def finish(i, c, k=k):
            copy_of(k, i).wait()
            return c

        each_peer(axis, sizes, finish)


def exchange(operands, plan, number):
    sizes = {axis: lax.axis_size(axis) for axis, _ in plan}
    shapes = []
    for array, (axis, scattered) in zip(operands, plan):
        shape = array.shape if scattered else (sizes[axis],) + array.shape
        shapes.append(jax.ShapeDtypeStruct(shape, array.dtype))
    sems = [pltpu.SemaphoreType.DMA((sizes[axis],)) for axis, _ in plan]
    traffic = 2 * sum(s.size * s.dtype.itemsize for s in shapes)
    return pl.pallas_call(
        functools.partial(exchange_kernel, plan, sizes),
        out_shape=shapes,
        in_specs=[pl.BlockSpec(memory_space=pl.ANY)] * len(plan),
        out_specs=[pl.BlockSpec(memory_space=pl.ANY)] * len(plan),
        scratch_shapes=sems + sems + [pltpu.SemaphoreType.DMA((len(plan),))],
        compiler_params=pltpu.CompilerParams(collective_id=number, has_side_effects=True),
        cost_estimate=pl.CostEstimate(
            flops=0, bytes_accessed=16 * traffic, transcendentals=0
        ),
    )(*operands)


def rotate_heads(heads_in, gain_row, positions):
    values32 = heads_in.astype(jnp.float32)
    scaled = (
        values32
        * lax.rsqrt(jnp.mean(values32 * values32, axis=-1, keepdims=True) + epsilon)
        * gain_row
    )
    pair_count = scaled.shape[-1] // 4
    inv_freq = rotary_base ** (-jnp.arange(pair_count, dtype=jnp.float32) / pair_count)
    grid_row = (positions // GRID_W).astype(jnp.float32)
    grid_col = (positions % GRID_W).astype(jnp.float32)
    angles = jnp.concatenate([grid_row[:, None] * inv_freq, grid_col[:, None] * inv_freq], axis=-1)[
        :, None, :
    ]
    cosine = jnp.cos(angles)
    sine_part = jnp.sin(angles)
    first_half = scaled[..., 0::2]
    second_half = scaled[..., 1::2]
    turned = jnp.stack(
        [
            first_half * cosine - second_half * sine_part,
            first_half * sine_part + second_half * cosine,
        ],
        axis=-1,
    )
    return turned.reshape(scaled.shape).astype(jnp.bfloat16)


def span_length(row_count):
    length = min(row_count, 2048)
    while row_count % length:
        length -= 1
    return length


def rotated(query_rows, key_rows, value_rows, query_gain, key_gain):
    row_count = query_rows.shape[0]
    head_size = query_gain.shape[0]
    q_heads = query_rows.shape[1] // head_size
    kv_heads = key_rows.shape[1] // head_size
    positions = lax.axis_index("ep") * row_count + jnp.arange(row_count, dtype=jnp.int32)
    q_rot = rotate_heads(query_rows.reshape(row_count, q_heads, head_size), query_gain, positions)
    k_rot = rotate_heads(key_rows.reshape(row_count, kv_heads, head_size), key_gain, positions)
    key_value = jnp.stack([k_rot, value_rows.reshape(row_count, kv_heads, head_size)], axis=2)
    return q_rot, key_value.reshape(row_count, kv_heads * 2 * head_size)


def attend(q_rot, piece_rows):
    row_count, q_heads, head_size = q_rot.shape
    kv_heads = piece_rows.shape[1] // (2 * head_size)
    group = q_heads // kv_heads
    scale = head_size ** (-0.5)
    q_grouped = q_rot.reshape(row_count, kv_heads, group, head_size).transpose(1, 2, 0, 3)
    q_grouped = q_grouped.reshape(kv_heads, group * row_count, head_size)
    query_count = group * row_count
    initial = (
        jnp.full((kv_heads, query_count), -jnp.inf, jnp.float32),
        jnp.zeros((kv_heads, query_count), jnp.float32),
        jnp.zeros((kv_heads, query_count, head_size), jnp.float32),
    )

    def one_span(carried, span_rows):
        run_max, run_sum, mixed = carried
        keys_span = span_rows[:, :, 0, :]
        values_span = span_rows[:, :, 1, :]
        scores = (
            jnp.einsum("hrd,shd->hrs", q_grouped, keys_span, preferred_element_type=jnp.float32)
            * scale
        )
        new_max = jnp.maximum(run_max, jnp.max(scores, axis=-1))
        factor = jnp.exp(run_max - new_max)
        weights = jnp.exp(scores - new_max[..., None])
        run_sum = run_sum * factor + jnp.sum(weights, axis=-1)
        added = jnp.einsum(
            "hrs,shd->hrd",
            weights.astype(jnp.bfloat16),
            values_span,
            preferred_element_type=jnp.float32,
        )
        mixed = mixed * factor[..., None] + added
        return ((new_max, run_sum, mixed), None)

    piece_count = piece_rows.shape[0]
    length = span_length(piece_count)
    spans = piece_rows.reshape(piece_count // length, length, kv_heads, 2, head_size)
    carried, unused = lax.scan(one_span, initial, spans)
    run_max, run_sum, mixed = carried
    result = (mixed / run_sum[..., None]).astype(jnp.bfloat16)
    result = result.reshape(kv_heads, group, row_count, head_size).transpose(2, 0, 1, 3)
    return result.reshape(row_count, q_heads * head_size)


def slot_numbers(own_routes, experts, capacity):
    tok_rows = own_routes.shape[0]
    named = own_routes[:, :, None] == jnp.arange(experts, dtype=jnp.int32)
    counts = jnp.any(named, axis=1).astype(jnp.bfloat16)
    rows = jnp.arange(tok_rows, dtype=jnp.int32)
    before = (rows[:, None] > rows[None, :]).astype(jnp.bfloat16)
    earlier = jnp.dot(before, counts, preferred_element_type=jnp.float32)
    ranks = jnp.sum(jnp.where(named, earlier[:, None, :], 0.0), axis=2).astype(jnp.int32)
    return own_routes * capacity + ranks


def hidden_of(rows_in, w_gate, w_up):
    gate_proj = jnp.einsum("...rd,...df->...rf", rows_in, w_gate, preferred_element_type=jnp.float32)
    up_proj = jnp.einsum("...rd,...df->...rf", rows_in, w_up, preferred_element_type=jnp.float32)
    return lax.optimization_barrier((jax.nn.silu(gate_proj) * up_proj).astype(jnp.bfloat16))


def body(
    query_rows,
    key_rows,
    value_rows,
    query_gain,
    key_gain,
    moe_tokens,
    norm_gain,
    routes,
    route_weights,
    expert_gate,
    expert_up,
    expert_down,
    shared_gate,
    shared_up,
    shared_down,
):
    tok_rows, model_width = moe_tokens.shape
    top_count = routes.shape[1]
    tp_size = lax.axis_size("tp")
    ep_size = lax.axis_size("ep")
    local_experts = expert_gate.shape[0]
    experts = local_experts * ep_size
    capacity = 2 * tok_rows * top_count // experts
    lane = lax.axis_index("tp")

    all_gate, _ = doubled([expert_gate], "tp")
    all_up, _ = doubled([expert_up], "tp")
    all_down, _ = doubled([expert_down], "tp")

    values32 = moe_tokens.astype(jnp.float32)
    normed = (
        values32
        * lax.rsqrt(jnp.mean(values32 * values32, axis=-1, keepdims=True) + epsilon)
        * norm_gain
    ).astype(jnp.bfloat16)
    own_routes = lax.dynamic_slice_in_dim(routes, lane * tok_rows, tok_rows, 0)
    own_weights = lax.dynamic_slice_in_dim(route_weights, lane * tok_rows, tok_rows, 0)
    own_gates = own_weights / jnp.sum(own_weights, axis=-1, keepdims=True) * routed_scale
    slots = slot_numbers(own_routes, experts, capacity)
    slot_ids = jnp.arange(experts * capacity, dtype=jnp.int32)
    placing = jnp.any(slot_ids[:, None, None] == slots[None, :, :], axis=2).astype(jnp.bfloat16)
    send = jnp.dot(placing, normed, preferred_element_type=jnp.float32).astype(jnp.bfloat16)
    send = send.reshape(ep_size, local_experts * capacity, model_width)

    q_rot, key_value = rotated(query_rows, key_rows, value_rows, query_gain, key_gain)

    group_rows, masks = doubled([normed], "tp")
    arrived, pieces = exchange((send, key_value), (("ep", True), ("ep", False)), 1)
    attn_out = attend(q_rot, pieces.reshape(-1, pieces.shape[-1]))
    group_rows = jnp.concatenate([group_rows[masks.index(i)] for i in range(tp_size)], axis=0)
    shared_hidden = hidden_of(group_rows, shared_gate, shared_up)
    shared_part = jnp.dot(shared_hidden, shared_down, preferred_element_type=jnp.float32)
    shared_part = shared_part.astype(jnp.bfloat16).reshape(tp_size, tok_rows, model_width)

    arrived = arrived.reshape(ep_size, local_experts, capacity, model_width).transpose(1, 0, 2, 3)
    arrived = arrived.reshape(local_experts, ep_size * capacity, model_width)
    total = 0.0
    for part in range(tp_size):
        hidden = hidden_of(arrived, all_gate[part], all_up[part])
        partial = jnp.einsum(
            "lrf,lfd->lrd", hidden, all_down[part], preferred_element_type=jnp.float32
        )
        total = total + partial.astype(jnp.bfloat16).astype(jnp.float32)
    outgoing = total.astype(jnp.bfloat16).reshape(local_experts, ep_size, capacity, model_width)
    outgoing = outgoing.transpose(1, 0, 2, 3).reshape(
        ep_size, local_experts * capacity, model_width
    )
    returned, shared_parts = exchange((outgoing, shared_part), (("ep", True), ("tp", True)), 2)

    flat_rows = returned.reshape(experts * capacity, model_width)
    moe_out = jnp.sum(shared_parts.astype(jnp.float32), axis=0)
    for k in range(top_count):
        choosing = (slots[:, k, None] == slot_ids[None, :]).astype(jnp.bfloat16)
        picked = jnp.dot(choosing, flat_rows, preferred_element_type=jnp.float32)
        moe_out = moe_out + own_gates[:, k, None] * picked
    return (attn_out, moe_out.astype(jnp.bfloat16))


def solution(mesh):
    return jax.shard_map(
        body,
        mesh=mesh,
        in_specs=(
            P("ep", "tp"),
            P("ep", "tp"),
            P("ep", "tp"),
            P(),
            P(),
            P(("ep", "tp"), None),
            P(),
            P("ep", None),
            P("ep", None),
            P("ep", None, "tp"),
            P("ep", None, "tp"),
            P("ep", "tp", None),
            P(None, "tp"),
            P(None, "tp"),
            P("tp", None),
        ),
        out_specs=(P("ep", "tp"), P(("ep", "tp"), None)),
        check_vma=False,
    )
```

```python
import functools

import jax
import jax.numpy as jnp
from jax import lax
from jax.experimental import pallas as pl
from jax.experimental.pallas import tpu as pltpu
from jax.sharding import PartitionSpec as P

GRID_W = 64


epsilon = 1e-06
rotary_base = 10000.0
routed_scale = 2.5


def doubled(blocks, axis):
    n = lax.axis_size(axis)
    masks, step = [0], n // 2
    while step:
        pairs = [(j, j ^ step) for j in range(n)]
        blocks = blocks + [lax.ppermute(block, axis, pairs) for block in blocks]
        masks = masks + [mask ^ step for mask in masks]
        step //= 2
    return blocks, masks


def swapped(block, axis, mask):
    if mask == 0:
        return block
    pairs = [(j, j ^ mask) for j in range(lax.axis_size(axis))]
    return lax.ppermute(block, axis, pairs)


def expert_kernel(parts, blocks, tile, *refs):
    arrived = refs[:blocks]
    gates, ups, downs = (refs[blocks + k * parts : blocks + (k + 1) * parts] for k in range(3))
    outs = refs[blocks + 3 * parts : 2 * blocks + 3 * parts]
    rows_in, gate_buf, up_buf, down_buf, total, sems = refs[2 * blocks + 3 * parts :]
    copies = []
    for part in range(parts):
        for k, (source, buf) in enumerate(
            ((gates[part], gate_buf), (ups[part], up_buf), (downs[part], down_buf))
        ):
            copy = pltpu.make_async_copy(source, buf.at[part], sems.at[part, k])
            copy.start()
            copies.append(copy)
    rows = arrived[0].shape[0]
    width = total.shape[1]
    for i in range(blocks):
        rows_in[pl.ds(i * rows, rows), :] = arrived[i][...]
    for part in range(parts):
        copies[3 * part].wait()
        gate_proj = jnp.dot(rows_in[...], gate_buf[part], preferred_element_type=jnp.float32)
        copies[3 * part + 1].wait()
        up_proj = jnp.dot(rows_in[...], up_buf[part], preferred_element_type=jnp.float32)
        hidden = (gate_proj / (1.0 + jnp.exp(-gate_proj)) * up_proj).astype(jnp.bfloat16)
        copies[3 * part + 2].wait()
        for at in range(0, width, tile):
            partial = jnp.dot(
                hidden, down_buf[part, :, at : at + tile], preferred_element_type=jnp.float32
            )
            partial = partial.astype(jnp.bfloat16).astype(jnp.float32)
            if part > 0:
                partial = partial + total[:, at : at + tile]
            if part < parts - 1:
                total[:, at : at + tile] = partial
            else:
                for i in range(blocks):
                    outs[i][:, at : at + tile] = partial[i * rows : (i + 1) * rows].astype(
                        jnp.bfloat16
                    )


def expert_rows(arrived, gates, ups, downs):
    blocks, parts = len(arrived), len(gates)
    rows, width = arrived[0].shape
    units = gates[0].shape[1]
    vmem, anywhere = pl.BlockSpec(memory_space=pltpu.VMEM), pl.BlockSpec(memory_space=pl.ANY)
    total = blocks * rows
    return pl.pallas_call(
        functools.partial(expert_kernel, parts, blocks, min(512, width)),
        out_shape=[jax.ShapeDtypeStruct((rows, width), jnp.bfloat16)] * blocks,
        in_specs=[vmem] * blocks + [anywhere] * (3 * parts),
        out_specs=[vmem] * blocks,
        scratch_shapes=[
            pltpu.VMEM((total, width), jnp.bfloat16),
            pltpu.VMEM((parts, width, units), jnp.bfloat16),
            pltpu.VMEM((parts, width, units), jnp.bfloat16),
            pltpu.VMEM((parts, units, width), jnp.bfloat16),
            pltpu.VMEM((total, width), jnp.float32),
            pltpu.SemaphoreType.DMA((parts, 3)),
        ],
        compiler_params=pltpu.CompilerParams(vmem_limit_bytes=40 * 1024 * 1024),
        cost_estimate=pl.CostEstimate(
            flops=6 * total * width * units * parts,
            bytes_accessed=2 * (3 * parts * width * units + 2 * total * width),
            transcendentals=total * units * parts,
        ),
    )(*arrived, *gates, *ups, *downs)


def rotate_heads(heads_in, gain_row, positions):
    values32 = heads_in.astype(jnp.float32)
    scaled = (
        values32
        * lax.rsqrt(jnp.mean(values32 * values32, axis=-1, keepdims=True) + epsilon)
        * gain_row
    )
    pair_count = scaled.shape[-1] // 4
    inv_freq = rotary_base ** (-jnp.arange(pair_count, dtype=jnp.float32) / pair_count)
    grid_row = (positions // GRID_W).astype(jnp.float32)
    grid_col = (positions % GRID_W).astype(jnp.float32)
    angles = jnp.concatenate([grid_row[:, None] * inv_freq, grid_col[:, None] * inv_freq], axis=-1)[
        :, None, :
    ]
    cosine = jnp.cos(angles)
    sine_part = jnp.sin(angles)
    first_half = scaled[..., 0::2]
    second_half = scaled[..., 1::2]
    turned = jnp.stack(
        [
            first_half * cosine - second_half * sine_part,
            first_half * sine_part + second_half * cosine,
        ],
        axis=-1,
    )
    return turned.reshape(scaled.shape).astype(jnp.bfloat16)


def span_length(row_count):
    length = min(row_count, 2048)
    while row_count % length:
        length -= 1
    return length


def rotated(query_rows, key_rows, value_rows, query_gain, key_gain):
    row_count = query_rows.shape[0]
    head_size = query_gain.shape[0]
    q_heads = query_rows.shape[1] // head_size
    kv_heads = key_rows.shape[1] // head_size
    positions = lax.axis_index("ep") * row_count + jnp.arange(row_count, dtype=jnp.int32)
    q_rot = rotate_heads(query_rows.reshape(row_count, q_heads, head_size), query_gain, positions)
    k_rot = rotate_heads(key_rows.reshape(row_count, kv_heads, head_size), key_gain, positions)
    key_value = jnp.stack([k_rot, value_rows.reshape(row_count, kv_heads, head_size)], axis=2)
    return q_rot, key_value.reshape(row_count, kv_heads * 2 * head_size)


def attend(q_rot, piece_rows):
    row_count, q_heads, head_size = q_rot.shape
    kv_heads = piece_rows.shape[1] // (2 * head_size)
    group = q_heads // kv_heads
    scale = head_size ** (-0.5)
    q_grouped = q_rot.reshape(row_count, kv_heads, group, head_size).transpose(1, 2, 0, 3)
    q_grouped = q_grouped.reshape(kv_heads, group * row_count, head_size)
    query_count = group * row_count
    initial = (
        jnp.full((kv_heads, query_count), -jnp.inf, jnp.float32),
        jnp.zeros((kv_heads, query_count), jnp.float32),
        jnp.zeros((kv_heads, query_count, head_size), jnp.float32),
    )

    def one_span(carried, span_rows):
        run_max, run_sum, mixed = carried
        keys_span = span_rows[:, :, 0, :]
        values_span = span_rows[:, :, 1, :]
        scores = (
            jnp.einsum("hrd,shd->hrs", q_grouped, keys_span, preferred_element_type=jnp.float32)
            * scale
        )
        new_max = jnp.maximum(run_max, jnp.max(scores, axis=-1))
        factor = jnp.exp(run_max - new_max)
        weights = jnp.exp(scores - new_max[..., None])
        run_sum = run_sum * factor + jnp.sum(weights, axis=-1)
        added = jnp.einsum(
            "hrs,shd->hrd",
            weights.astype(jnp.bfloat16),
            values_span,
            preferred_element_type=jnp.float32,
        )
        mixed = mixed * factor[..., None] + added
        return ((new_max, run_sum, mixed), None)

    piece_count = piece_rows.shape[0]
    length = span_length(piece_count)
    spans = piece_rows.reshape(piece_count // length, length, kv_heads, 2, head_size)
    carried, unused = lax.scan(one_span, initial, spans)
    run_max, run_sum, mixed = carried
    result = (mixed / run_sum[..., None]).astype(jnp.bfloat16)
    result = result.reshape(kv_heads, group, row_count, head_size).transpose(2, 0, 1, 3)
    return result.reshape(row_count, q_heads * head_size)


def slot_numbers(own_routes, experts, capacity):
    tok_rows = own_routes.shape[0]
    named = own_routes[:, :, None] == jnp.arange(experts, dtype=jnp.int32)
    counts = jnp.any(named, axis=1).astype(jnp.bfloat16)
    rows = jnp.arange(tok_rows, dtype=jnp.int32)
    before = (rows[:, None] > rows[None, :]).astype(jnp.bfloat16)
    earlier = jnp.dot(before, counts, preferred_element_type=jnp.float32)
    ranks = jnp.sum(jnp.where(named, earlier[:, None, :], 0.0), axis=2).astype(jnp.int32)
    return own_routes * capacity + ranks


def hidden_of(rows_in, w_gate, w_up):
    gate_proj = jnp.einsum("...rd,...df->...rf", rows_in, w_gate, preferred_element_type=jnp.float32)
    up_proj = jnp.einsum("...rd,...df->...rf", rows_in, w_up, preferred_element_type=jnp.float32)
    return lax.optimization_barrier((jax.nn.silu(gate_proj) * up_proj).astype(jnp.bfloat16))


def body(
    query_rows,
    key_rows,
    value_rows,
    query_gain,
    key_gain,
    moe_tokens,
    norm_gain,
    routes,
    route_weights,
    expert_gate,
    expert_up,
    expert_down,
    shared_gate,
    shared_up,
    shared_down,
):
    tok_rows, model_width = moe_tokens.shape
    top_count = routes.shape[1]
    tp_size = lax.axis_size("tp")
    ep_size = lax.axis_size("ep")
    local_experts = expert_gate.shape[0]
    experts = local_experts * ep_size
    capacity = 2 * tok_rows * top_count // experts
    lane = lax.axis_index("tp")

    me = lax.axis_index("ep")
    nearness = list(range(ep_size))[::-1]
    all_gate, _ = doubled([expert_gate], "tp")
    all_up, _ = doubled([expert_up], "tp")
    all_down, _ = doubled([expert_down], "tp")

    values32 = moe_tokens.astype(jnp.float32)
    normed = (
        values32
        * lax.rsqrt(jnp.mean(values32 * values32, axis=-1, keepdims=True) + epsilon)
        * norm_gain
    ).astype(jnp.bfloat16)
    own_routes = lax.dynamic_slice_in_dim(routes, lane * tok_rows, tok_rows, 0)
    own_weights = lax.dynamic_slice_in_dim(route_weights, lane * tok_rows, tok_rows, 0)
    own_gates = own_weights / jnp.sum(own_weights, axis=-1, keepdims=True) * routed_scale
    near_routes = (own_routes // local_experts ^ me) * local_experts + own_routes % local_experts
    slots = slot_numbers(near_routes, experts, capacity)
    slot_ids = jnp.arange(experts * capacity, dtype=jnp.int32)
    block_slots = local_experts * capacity
    arrived = [None] * ep_size
    in_turn = normed
    for i in nearness:
        ids = i * block_slots + jnp.arange(block_slots, dtype=jnp.int32)
        placing = jnp.any(ids[:, None, None] == slots[None, :, :], axis=2).astype(jnp.bfloat16)
        send = jnp.dot(placing, in_turn, preferred_element_type=jnp.float32).astype(jnp.bfloat16)
        in_turn, send = lax.optimization_barrier((in_turn, send))
        arrived[i] = swapped(send, "ep", i)
    group_rows, masks = doubled([normed], "tp")

    q_rot, pieces = rotated(query_rows, key_rows, value_rows, query_gain, key_gain)
    step = ep_size // 2
    while step:
        pieces = jnp.concatenate([pieces, swapped(pieces, "ep", step)], axis=0)
        step //= 2
    attn_out = attend(q_rot, pieces)

    shared_sum = 0.0
    for rows_in, mask in zip(group_rows, masks):
        shared_hidden = hidden_of(rows_in, shared_gate, shared_up)
        shared_part = jnp.dot(shared_hidden, shared_down, preferred_element_type=jnp.float32)
        part_in = swapped(shared_part.astype(jnp.bfloat16), "tp", mask)
        shared_sum = shared_sum + part_in.astype(jnp.float32)

    returned = [None] * ep_size
    half = max(ep_size // 2, 1)
    for wanted in (list(range(half, ep_size)), list(range(half))):
        results = [[] for _ in wanted]
        for expert in range(local_experts):
            cut = slice(expert * capacity, (expert + 1) * capacity)
            done = expert_rows(
                [arrived[i][cut] for i in wanted],
                [w[expert] for w in all_gate],
                [w[expert] for w in all_up],
                [w[expert] for w in all_down],
            )
            for got, rows_out in zip(results, done):
                got.append(rows_out)
            done, arrived = lax.optimization_barrier((done, arrived))
        for i, got in sorted(zip(wanted, results), key=lambda pair: -pair[0]):
            block = got[0] if local_experts == 1 else jnp.concatenate(got, axis=0)
            returned[i] = swapped(block, "ep", i)

    flat_rows = jnp.concatenate(returned, axis=0)
    moe_out = shared_sum
    for k in range(top_count):
        choosing = (slots[:, k, None] == slot_ids[None, :]).astype(jnp.bfloat16)
        picked = jnp.dot(choosing, flat_rows, preferred_element_type=jnp.float32)
        moe_out = moe_out + own_gates[:, k, None] * picked
    return (attn_out, moe_out.astype(jnp.bfloat16))


def solution(mesh):
    return jax.shard_map(
        body,
        mesh=mesh,
        in_specs=(
            P("ep", "tp"),
            P("ep", "tp"),
            P("ep", "tp"),
            P(),
            P(),
            P(("ep", "tp"), None),
            P(),
            P("ep", None),
            P("ep", None),
            P("ep", None, "tp"),
            P("ep", None, "tp"),
            P("ep", "tp", None),
            P(None, "tp"),
            P(None, "tp"),
            P("tp", None),
        ),
        out_specs=(P("ep", "tp"), P(("ep", "tp"), None)),
        check_vma=False,
    )
```
